32 devices in a mesh: fs: 8 (over z, x), tp: 4 (over y, core).
Axes of the slice: x: 2, y: 2, z: 4, core: 2. Of those that a mesh axis runs over, the one named last changes fastest.
Arguments:
- layer_input: bfloat16 [6144, 2048], P('fs'), may hold values from -6 to 6
- branch_cotangent: bfloat16 [6144, 1024], P('fs', 'tp'), may hold values from -0.057373047 to 0.057373047
- gate_cotangent: bfloat16 [6144, 1024], P('fs', 'tp'), may hold values from -0.057373047 to 0.057373047
- branch_factor: bfloat16 [2048, 128], P('fs'), may hold values from -0.5 to 0.5
- gate_factor: bfloat16 [2048, 128], P('fs'), may hold values from -0.5 to 0.5
- branch_weight: float32 [2048, 1024], P('fs', 'tp'), may hold values from -6 to 6
- gate_weight: float32 [2048, 1024], P('fs', 'tp'), may hold values from -6 to 6
- branch_first: float32 [128, 1024], P(None, 'tp'), may hold values from -6 to 6
- gate_first: float32 [128, 1024], P(None, 'tp'), may hold values from -6 to 6
- branch_second: float32 [128, 1024], P(None, 'tp'), may hold values from 0.0625 to 900
- gate_second: float32 [128, 1024], P(None, 'tp'), may hold values from 0.0625 to 900
Outputs:
- branch_step: float32 [2048, 1024], P('fs', 'tp')
- gate_step: float32 [2048, 1024], P('fs', 'tp')
- branch_new: float32 [2048, 1024], P('fs', 'tp')
- gate_new: float32 [2048, 1024], P('fs', 'tp')
- branch_copy: bfloat16 [2048, 1024], P(None, 'tp')
- gate_copy: bfloat16 [2048, 1024], P(None, 'tp')
- branch_first_new: float32 [128, 1024], P(None, 'tp')
- gate_first_new: float32 [128, 1024], P(None, 'tp')
- branch_second_new: float32 [128, 1024], P(None, 'tp')
- gate_second_new: float32 [128, 1024], P(None, 'tp')
The draws below stay inside these ranges and needn't reach their ends.
All inputs are finite; a program needn't handle non-finite values.
Results may differ from the reference program's by a relative error of at most 0.00055.
Values may be sent and summed in bfloat16 or wider, within the bound.
A program may use at most 64 MiB of HBM per device.

```python
import jax
import jax.numpy as jnp
from jax import lax

D = 2048
W = 1024
RANK = 128
TOKENS = 6144


def second_moment(key, marker):
    base_key = jax.random.fold_in(key, marker)
    row_key, col_key, noise_key = jax.random.split(base_key, 3)
    columns = jnp.arange(W, dtype=jnp.float32) / (W - 1)
    col_scale = jnp.exp(1.2 * (1.0 - columns)) * jax.random.uniform(col_key, (W,), jnp.float32, 1.0, 3.0)
    row_scale = jax.random.uniform(row_key, (RANK,), jnp.float32, 1.0, 3.0)
    noise = jnp.exp(jax.random.uniform(noise_key, (RANK, W), jnp.float32, jnp.log(0.5), jnp.log(2.0)))
    outer = row_scale[:, None] * col_scale[None, :]
    return (0.25 * noise * outer * outer).astype(jnp.float32)


def draw_branch_second(key, part):
    return second_moment(key, 11)


def draw_gate_second(key, part):
    return second_moment(key, 12)


def level_of(stream_key, extent, shards, smallest, largest):
    gain = 1.0
    for axis_at, parts in shards:
        heights = jax.random.uniform(jax.random.fold_in(jax.random.fold_in(stream_key, 6), axis_at), (parts,), jnp.float32, smallest / len(shards), largest / len(shards))
        gain = gain * jnp.repeat(jnp.exp(heights), extent[axis_at] // parts).reshape((-1,) + (1,) * (len(extent) - 1 - axis_at))
    return gain


def gaussian(rng, dims, width, bound, pieces=(), kind=jnp.bfloat16):
    values = jax.random.normal(rng, dims, jnp.float32) * width
    if len(pieces) > 0:
        values = level_of(rng, dims, pieces, -0.22, 0.18) * values
    return jnp.clip(values, min=-bound, max=bound).astype(kind)


def setup_inputs(seed: int = 0) -> dict:
    arg_keys = jax.random.split(jax.random.key(seed), 12)
    layer_input = gaussian(arg_keys[0], (TOKENS, D), 1.0, 6.0, ((0, 8),))
    branch_cotangent = gaussian(arg_keys[1], (TOKENS, W), (0.75 * TOKENS ** -0.5), 0.057373047, ((0, 8), (1, 4)))
    gate_cotangent = gaussian(arg_keys[2], (TOKENS, W), (0.75 * TOKENS ** -0.5), 0.057373047, ((0, 8), (1, 4)))
    branch_factor = gaussian(arg_keys[3], (D, RANK), RANK ** -0.5, 0.5, ((0, 8),))
    gate_factor = gaussian(arg_keys[4], (D, RANK), RANK ** -0.5, 0.5, ((0, 8),))
    branch_weight = gaussian(arg_keys[5], (D, W), 1.0, 6.0, ((0, 8), (1, 4)), jnp.float32)
    gate_weight = gaussian(arg_keys[6], (D, W), 1.0, 6.0, ((0, 8), (1, 4)), jnp.float32)
    branch_first = gaussian(arg_keys[7], (RANK, W), 1.0, 6.0, ((1, 4),), jnp.float32)
    gate_first = gaussian(arg_keys[8], (RANK, W), 1.0, 6.0, ((1, 4),), jnp.float32)
    branch_second = draw_branch_second(jax.random.fold_in(arg_keys[11], 71), 0)
    gate_second = draw_gate_second(jax.random.fold_in(arg_keys[11], 71), 0)
    return dict(layer_input=layer_input, branch_cotangent=branch_cotangent, gate_cotangent=gate_cotangent, branch_factor=branch_factor, gate_factor=gate_factor, branch_weight=branch_weight, gate_weight=gate_weight, branch_first=branch_first, gate_first=gate_first, branch_second=branch_second, gate_second=gate_second)


first_decay = 0.8
second_decay = 0.9
learn_rate = 0.5

def reference(layer_input, branch_cotangent, gate_cotangent, branch_factor, gate_factor, branch_weight, gate_weight, branch_first, gate_first, branch_second, gate_second):
    highest = lax.Precision.HIGHEST
    groups = ((branch_cotangent, branch_factor, branch_first, branch_second), (gate_cotangent, gate_factor, gate_first, gate_second))
    firsts_new = []
    seconds_new = []
    directions = []
    sum_squares = jnp.zeros((), jnp.float32)
    for cotangent, factor, first_old, second_old in groups:
        gradient = jnp.dot(layer_input.T, cotangent, preferred_element_type=jnp.float32)
        projected = jnp.dot(factor.astype(jnp.float32).T, gradient, precision=highest)
        first_new = first_decay * first_old + (1.0 - first_decay) * projected
        second_new = second_decay * second_old + (1.0 - second_decay) * projected * projected
        direction = first_new / jnp.sqrt(second_new)
        sum_squares = sum_squares + jnp.sum(direction * direction)
        firsts_new.append(first_new)
        seconds_new.append(second_new)
        directions.append(direction)
    step_scale = learn_rate / jnp.sqrt(sum_squares / (2 * RANK * W) + 1e-06)
    branch_step = -step_scale * jnp.dot(branch_factor.astype(jnp.float32), directions[0], precision=highest)
    gate_step = -step_scale * jnp.dot(gate_factor.astype(jnp.float32), directions[1], precision=highest)
    branch_new = branch_weight + branch_step
    gate_new = gate_weight + gate_step
    return (branch_step, gate_step, branch_new, gate_new, branch_new.astype(jnp.bfloat16), gate_new.astype(jnp.bfloat16), firsts_new[0], firsts_new[1], seconds_new[0], seconds_new[1])
```

```python
import functools

import jax
import jax.numpy as jnp
from jax import lax
from jax.experimental import pallas as pl
from jax.experimental.pallas import tpu as pltpu
from jax.sharding import PartitionSpec as P

first_decay = 0.8
second_decay = 0.9
learn_rate = 0.5


def update_moments(projected, first_old, second_old):
    first_new = first_decay * first_old + (1.0 - first_decay) * projected
    second_new = second_decay * second_old + (1.0 - second_decay) * projected * projected
    return (first_new, second_new, first_new / jnp.sqrt(second_new))


def local(
    layer_input,
    branch_cotangent,
    gate_cotangent,
    branch_factor,
    gate_factor,
    branch_weight,
    gate_weight,
    branch_first,
    gate_first,
    branch_second,
    gate_second,
):
    highest = lax.Precision.HIGHEST
    width = branch_cotangent.shape[1]
    branch_whole, gate_whole = (
        lax.all_gather(branch_factor, "fs", axis=0, tiled=True),
        lax.all_gather(gate_factor, "fs", axis=0, tiled=True),
    )
    branch_rows = jnp.dot(layer_input, branch_whole, preferred_element_type=jnp.float32)
    gate_rows = jnp.dot(layer_input, gate_whole, preferred_element_type=jnp.float32)
    branch_local = jnp.einsum(
        "tr,tw->rw", branch_rows, branch_cotangent.astype(jnp.float32), precision=highest
    )
    gate_local = jnp.einsum(
        "tr,tw->rw", gate_rows, gate_cotangent.astype(jnp.float32), precision=highest
    )
    branch_projected, gate_projected = lax.psum((branch_local, gate_local), "fs")
    branch_first_new, branch_second_new, branch_direction = update_moments(
        branch_projected, branch_first, branch_second
    )
    gate_first_new, gate_second_new, gate_direction = update_moments(
        gate_projected, gate_first, gate_second
    )
    local_squares = jnp.sum(branch_direction * branch_direction) + jnp.sum(
        gate_direction * gate_direction
    )
    sum_squares = lax.psum(local_squares, "tp")
    entries = 2 * branch_direction.shape[0] * width * lax.axis_size("tp")
    step_scale = learn_rate / jnp.sqrt(sum_squares / entries + 1e-06)
    branch_step = -step_scale * jnp.dot(
        branch_factor.astype(jnp.float32), branch_direction, precision=highest
    )
    gate_step = -step_scale * jnp.dot(
        gate_factor.astype(jnp.float32), gate_direction, precision=highest
    )
    branch_new = branch_weight + branch_step
    gate_new = gate_weight + gate_step
    branch_copy, gate_copy = (
        lax.all_gather(branch_new.astype(jnp.bfloat16), "fs", axis=0, tiled=True),
        lax.all_gather(gate_new.astype(jnp.bfloat16), "fs", axis=0, tiled=True),
    )
    return (
        branch_step,
        gate_step,
        branch_new,
        gate_new,
        branch_copy,
        gate_copy,
        branch_first_new,
        gate_first_new,
        branch_second_new,
        gate_second_new,
    )


BF, F32 = jnp.bfloat16, jnp.float32


def parts(value, count):
    terms = []
    for _ in range(count):
        term = value.astype(BF)
        terms.append(term)
        value = value - term.astype(F32)
    return terms


def remote(src, dst, send_sem, recv_sem, **where):
    return pltpu.make_async_remote_copy(
        src_ref=src,
        dst_ref=dst,
        send_sem=send_sem,
        recv_sem=recv_sem,
        device_id=where,
        device_id_type=pl.DeviceIdType.MESH,
    )


class Line:
    def __init__(self, nf, me, piece, recv, up, down, across):
        self.nl = nf // 2
        self.me, self.z, self.x = me, me // 2, me % 2
        self.piece, self.recv = piece, recv
        self.sems = {"up": up, "down": down, "across": across}

    def copy(self, slot, way):
        target = {"up": self.me + 2, "down": self.me - 2, "across": self.me + 1 - 2 * self.x}[way]
        return remote(self.piece(slot), self.piece(slot), self.sems[way].at[slot], self.recv.at[slot], fs=target)

    def arrive(self, slot):
        self.copy(slot, "across").wait_recv()

    def open(self):
        @pl.when(self.z < self.nl - 1)
        def _():
            self.copy(self.me, "up").start()

        @pl.when(self.z > 0)
        def _():
            self.copy(self.me, "down").start()

        self.copy(self.me, "across").start()

    def step(self, dist, then=lambda slot: None):
        @pl.when(self.z >= dist)
        def _():
            slot = self.me - 2 * dist
            self.arrive(slot)

            @pl.when(self.z < self.nl - 1)
            def _():
                self.copy(slot, "up").start()

            self.copy(slot, "across").start()
            then(slot)

        @pl.when(self.z + dist < self.nl)
        def _():
            slot = self.me + 2 * dist
            self.arrive(slot)

            @pl.when(self.z > 0)
            def _():
                self.copy(slot, "down").start()

            self.copy(slot, "across").start()
            then(slot)

    def other(self, dist, then=lambda slot: None):
        pair = self.me + 1 - 2 * self.x
        if dist == 0:
            self.arrive(pair)
            then(pair)
            return

        @pl.when(self.z >= dist)
        def _():
            self.arrive(pair - 2 * dist)
            then(pair - 2 * dist)

        @pl.when(self.z + dist < self.nl)
        def _():
            self.arrive(pair + 2 * dist)
            then(pair + 2 * dist)

    def close(self):
        for line in range(self.nl):
            slot = 2 * line + self.x

            @pl.when((self.z >= line) & (self.z < self.nl - 1))
            def _():
                self.copy(slot, "up").wait_send()

            @pl.when((self.z <= line) & (self.z > 0))
            def _():
                self.copy(slot, "down").wait_send()

            self.copy(slot, "across").wait_send()


def main_kernel(nf, nt, *refs):
    x_in, c_in, f_in, w_in = refs[0], refs[1:3], refs[3:5], refs[5:7]
    first_in, second_in = refs[7:9], refs[9:11]
    step_out, new_out, copy_out, first_out, second_out = (refs[i : i + 2] for i in range(11, 21, 2))
    (xv, cv, fbuf, rl, rs, rfull, ss, wv, m1, m2, stv, nwv, fnv, snv, cbuf) = refs[21:36]
    (in_sem, out_sem, f_sem, core_sem, rs_sem, ag_sem, ss_sem, cp_sem, co_sem) = refs[36:]
    me, tp = lax.axis_index("fs"), lax.axis_index("tp")
    depth = f_in[0].shape[0]
    rank = f_in[0].shape[1]
    half = depth // 2
    core = tp % 2
    mate = tp + 1 - 2 * core
    pr = rs.shape[1]

    def block(slot):
        return pl.ds(pl.multiple_of(slot * depth, depth), depth)

    loads = [pltpu.make_async_copy(f_in[p], fbuf.at[block(me), pl.ds(p * rank, rank)], in_sem.at[p]) for p in range(2)]
    loads += [pltpu.make_async_copy(x_in, xv, in_sem.at[2])]
    for i, (src, dst) in enumerate(((c_in, cv), (first_in, m1), (second_in, m2), (w_in, wv))):
        loads += [pltpu.make_async_copy(src[p], dst.at[p], in_sem.at[3 + 2 * i + p]) for p in range(2)]
    for load in loads:
        load.start()

    barrier = pltpu.get_barrier_semaphore()
    for k in range(1, nf):
        pl.semaphore_signal(barrier, inc=1, device_id={"fs": (me + k) % nf}, device_id_type=pl.DeviceIdType.MESH)
    for k in range(1, nt):
        pl.semaphore_signal(barrier, inc=1, device_id={"tp": (tp + k) % nt}, device_id_type=pl.DeviceIdType.MESH)
    pl.semaphore_wait(barrier, nf + nt - 2)

    def half_of(slot, which):
        return fbuf.at[pl.ds(pl.multiple_of(slot * depth + which * half, half), half), :]

    gather = Line(nf, me, lambda slot: half_of(slot, core), f_sem.at[0], f_sem.at[1], f_sem.at[2], f_sem.at[3])

    def hand(slot):
        view = half_of(slot, core)
        return remote(view, view, core_sem.at[0, slot], core_sem.at[1, slot], tp=mate)

    def take(slot):
        view = half_of(slot, 1 - core)
        remote(view, view, core_sem.at[0, slot], core_sem.at[1, slot], tp=mate).wait_recv()

    loads[0].wait()
    loads[1].wait()
    gather.open()
    pass_on = lambda slot: hand(slot).start()
    gather.other(0, pass_on)
    for dist in range(1, nf // 2):
        gather.step(dist, pass_on)
        gather.other(dist, pass_on)
    for load in loads[2:5]:
        load.wait()
    for k in range(1, nf):
        take((me + k) % nf)

    rows = jnp.dot(xv[...], fbuf[...], preferred_element_type=F32)
    terms = parts(rows, 2)
    for p in range(2):
        total = 0.0
        for term in terms:
            total = total + lax.dot_general(
                term[:, p * rank : (p + 1) * rank], cv[p], (((0,), (0,)), ((), ())), preferred_element_type=F32
            )
        rl[p * rank : (p + 1) * rank, :] = total

    def piece(slot):
        return pl.ds(pl.multiple_of(slot * pr, pr), pr)

    def scatter(k):
        to = (me + k) % nf
        return remote(rl.at[piece(to), :], rs.at[me], rs_sem.at[0, k], rs_sem.at[1, me], fs=to)

    for k in range(1, nf):
        scatter(k).start()
    summed = rl[piece(me), :]
    for k in range(1, nf):
        frm = (me + k) % nf
        remote(rl.at[piece(me), :], rs.at[frm], rs_sem.at[0, k], rs_sem.at[1, frm], fs=frm).wait_recv()
        summed = summed + rs[frm]
    rfull[piece(me), :] = summed

    def spread(k):
        view = rfull.at[piece(me), :]
        return remote(view, view, ag_sem.at[0, k], ag_sem.at[1, me], fs=(me + k) % nf)

    for k in range(1, nf):
        spread(k).start()
    for load in loads[5:]:
        load.wait()
    for k in range(1, nf):
        frm = (me + k) % nf
        view = rfull.at[piece(frm), :]
        remote(view, view, ag_sem.at[0, k], ag_sem.at[1, frm], fs=frm).wait_recv()

    squares = jnp.zeros((), F32)
    directions = []
    for p in range(2):
        projected = rfull[p * rank : (p + 1) * rank, :]
        first_new, second_new, direction = update_moments(projected, m1[p], m2[p])
        fnv[p] = first_new
        snv[p] = second_new
        squares = squares + jnp.sum(direction * direction)
        directions.append(direction)
    ss[tp] = jnp.full(ss.shape[1:], squares, F32)

    def tell(k):
        return remote(ss.at[tp], ss.at[tp], ss_sem.at[0, k], ss_sem.at[1, tp], tp=(tp + k) % nt)

    for k in range(1, nt):
        tell(k).start()
    raw = []
    for p in range(2):
        own = fbuf[block(me), p * rank : (p + 1) * rank]
        total = 0.0
        for term in reversed(parts(directions[p], 3)):
            total = total + jnp.dot(own, term, preferred_element_type=F32)
        raw.append(total)
    for k in range(1, nt):
        frm = (tp + k) % nt
        remote(ss.at[frm], ss.at[frm], ss_sem.at[0, k], ss_sem.at[1, frm], tp=frm).wait_recv()
    total = ss[0]
    for t in range(1, nt):
        total = total + ss[t]
    entries = 2 * rank * directions[0].shape[1] * nt
    scale = (learn_rate / jnp.sqrt(total / entries + 1e-06))[0:1, 0:1]

    lines = []
    for p in range(2):
        step = -scale * raw[p]
        stv[p] = step
        new = wv[p] + step
        nwv[p] = new
        cbuf[p, block(me), :] = new.astype(BF)
        lines.append(
            Line(
                nf,
                me,
                functools.partial(lambda p, slot: cbuf.at[p, block(slot), :], p),
                cp_sem.at[p, 0],
                cp_sem.at[p, 1],
                cp_sem.at[p, 2],
                cp_sem.at[p, 3],
            )
        )
        lines[p].open()
    outs = []
    for i, (src, dst) in enumerate(((fnv, first_out), (snv, second_out), (stv, step_out), (nwv, new_out))):
        outs += [pltpu.make_async_copy(src.at[p], dst[p], out_sem.at[2 * i + p]) for p in range(2)]
    for out in outs:
        out.start()

    def put(p, slot):
        return pltpu.make_async_copy(cbuf.at[p, block(slot), :], copy_out[p].at[block(slot), :], co_sem.at[p, slot])

    starts = [functools.partial(lambda p, slot: put(p, slot).start(), p) for p in range(2)]
    for p in range(2):
        starts[p](me)
    for dist in range(1, nf // 2):
        for p in range(2):
            lines[p].step(dist, starts[p])
        for p in range(2):
            lines[p].other(dist - 1, starts[p])
    for p in range(2):
        lines[p].other(nf // 2 - 1, starts[p])

    gather.close()
    for line in lines:
        line.close()
    for k in range(1, nf):
        hand((me + k) % nf).wait_send()
        scatter(k).wait_send()
        spread(k).wait_send()
    for k in range(1, nt):
        tell(k).wait_send()
    for out in outs:
        out.wait()
    for p in range(2):
        for slot in range(nf):
            put(p, slot).wait()


def out_kernel(n, *refs):
    srcs, dsts, bufs, sems = refs[:n], refs[n : 2 * n], refs[2 * n : 3 * n], refs[3 * n]
    for i in range(n):
        pltpu.make_async_copy(srcs[i], bufs[i], sems.at[0, i]).start()
    for i in range(n):
        pltpu.make_async_copy(srcs[i], bufs[i], sems.at[0, i]).wait()
        pltpu.make_async_copy(bufs[i], dsts[i], sems.at[1, i]).start()
    for i in range(n):
        pltpu.make_async_copy(bufs[i], dsts[i], sems.at[1, i]).wait()


def fused(nf, nt, *args):
    x, cot, factor, weight, first = args[0], args[1], args[3], args[5], args[7]
    tokens, width = cot.shape
    depth, rank = factor.shape
    pr = 2 * rank // nf
    shape = jax.ShapeDtypeStruct
    outs = [shape(weight.shape, F32)] * 4 + [shape((nf * depth, width), BF)] * 2 + [shape(first.shape, F32)] * 4
    anywhere = pl.BlockSpec(memory_space=pl.ANY)
    vmem, dma = pltpu.VMEM, pltpu.SemaphoreType.DMA
    results = pl.pallas_call(
        functools.partial(main_kernel, nf, nt),
        out_shape=outs,
        in_specs=[anywhere] * 11,
        out_specs=[anywhere] * 10,
        scratch_shapes=[
            vmem(x.shape, BF),
            vmem((2, tokens, width), BF),
            vmem((nf * depth, 2 * rank), BF),
            vmem((2 * rank, width), F32),
            vmem((nf, pr, width), F32),
            vmem((2 * rank, width), F32),
            vmem((nt, 8, 128), F32),
            vmem((2, depth, width), F32),
            vmem((2, rank, width), F32),
            vmem((2, rank, width), F32),
            vmem((2, depth, width), F32),
            vmem((2, depth, width), F32),
            vmem((2, rank, width), F32),
            vmem((2, rank, width), F32),
            vmem((2, nf * depth, width), BF),
            dma((11,)),
            dma((8,)),
            dma((4, nf)),
            dma((2, nf)),
            dma((2, nf)),
            dma((2, nf)),
            dma((2, nt)),
            dma((2, 4, nf)),
            dma((2, nf)),
        ],
        compiler_params=pltpu.CompilerParams(
            collective_id=0, has_side_effects=True, vmem_limit_bytes=40 * 1024 * 1024
        ),
    )(*args)
    return pl.pallas_call(
        functools.partial(out_kernel, len(outs)),
        out_shape=outs,
        in_specs=[anywhere] * 10,
        out_specs=[anywhere] * 10,
        scratch_shapes=[vmem(o.shape, o.dtype) for o in outs] + [dma((2, len(outs)))],
    )(*results)


def fits(nf, nt, depth, rank):
    return nf % 2 == 0 and nt % 2 == 0 and nf <= 16 and depth % 32 == 0 and (2 * rank) % (8 * nf) == 0


def device_step(nf, nt, *args):
    depth, rank = args[3].shape
    if fits(nf, nt, depth, rank):
        return tuple(fused(nf, nt, *args))
    return local(*args)


def solution(mesh):
    return jax.shard_map(
        functools.partial(device_step, mesh.shape["fs"], mesh.shape["tp"]),
        mesh=mesh,
        in_specs=(
            P("fs", None),
            P("fs", "tp"),
            P("fs", "tp"),
            P("fs", None),
            P("fs", None),
            P("fs", "tp"),
            P("fs", "tp"),
            P(None, "tp"),
            P(None, "tp"),
            P(None, "tp"),
            P(None, "tp"),
        ),
        out_specs=(
            P("fs", "tp"),
            P("fs", "tp"),
            P("fs", "tp"),
            P("fs", "tp"),
            P(None, "tp"),
            P(None, "tp"),
            P(None, "tp"),
            P(None, "tp"),
            P(None, "tp"),
            P(None, "tp"),
        ),
        check_vma=False,
    )
```

```python
import functools

import jax
import jax.numpy as jnp
from jax import lax
from jax.experimental import pallas as pl
from jax.experimental.pallas import tpu as pltpu
from jax.sharding import PartitionSpec as P

first_decay = 0.8
second_decay = 0.9
learn_rate = 0.5


def update_moments(projected, first_old, second_old):
    first_new = first_decay * first_old + (1.0 - first_decay) * projected
    second_new = second_decay * second_old + (1.0 - second_decay) * projected * projected
    return (first_new, second_new, first_new / jnp.sqrt(second_new))


def local(
    layer_input,
    branch_cotangent,
    gate_cotangent,
    branch_factor,
    gate_factor,
    branch_weight,
    gate_weight,
    branch_first,
    gate_first,
    branch_second,
    gate_second,
):
    highest = lax.Precision.HIGHEST
    width = branch_cotangent.shape[1]
    branch_whole, gate_whole = (
        lax.all_gather(branch_factor, "fs", axis=0, tiled=True),
        lax.all_gather(gate_factor, "fs", axis=0, tiled=True),
    )
    branch_rows = jnp.dot(layer_input, branch_whole, preferred_element_type=jnp.float32)
    gate_rows = jnp.dot(layer_input, gate_whole, preferred_element_type=jnp.float32)
    branch_local = jnp.einsum(
        "tr,tw->rw", branch_rows, branch_cotangent.astype(jnp.float32), precision=highest
    )
    gate_local = jnp.einsum(
        "tr,tw->rw", gate_rows, gate_cotangent.astype(jnp.float32), precision=highest
    )
    branch_projected, gate_projected = lax.psum((branch_local, gate_local), "fs")
    branch_first_new, branch_second_new, branch_direction = update_moments(
        branch_projected, branch_first, branch_second
    )
    gate_first_new, gate_second_new, gate_direction = update_moments(
        gate_projected, gate_first, gate_second
    )
    local_squares = jnp.sum(branch_direction * branch_direction) + jnp.sum(
        gate_direction * gate_direction
    )
    sum_squares = lax.psum(local_squares, "tp")
    entries = 2 * branch_direction.shape[0] * width * lax.axis_size("tp")
    step_scale = learn_rate / jnp.sqrt(sum_squares / entries + 1e-06)
    branch_step = -step_scale * jnp.dot(
        branch_factor.astype(jnp.float32), branch_direction, precision=highest
    )
    gate_step = -step_scale * jnp.dot(
        gate_factor.astype(jnp.float32), gate_direction, precision=highest
    )
    branch_new = branch_weight + branch_step
    gate_new = gate_weight + gate_step
    branch_copy, gate_copy = (
        lax.all_gather(branch_new.astype(jnp.bfloat16), "fs", axis=0, tiled=True),
        lax.all_gather(gate_new.astype(jnp.bfloat16), "fs", axis=0, tiled=True),
    )
    return (
        branch_step,
        gate_step,
        branch_new,
        gate_new,
        branch_copy,
        gate_copy,
        branch_first_new,
        gate_first_new,
        branch_second_new,
        gate_second_new,
    )


BF, F32 = jnp.bfloat16, jnp.float32


def parts(value, count):
    terms = []
    for _ in range(count):
        term = value.astype(BF)
        terms.append(term)
        value = value - term.astype(F32)
    return terms


def remote(src, dst, send_sem, recv_sem, **where):
    return pltpu.make_async_remote_copy(
        src_ref=src,
        dst_ref=dst,
        send_sem=send_sem,
        recv_sem=recv_sem,
        device_id=where,
        device_id_type=pl.DeviceIdType.MESH,
    )


class Line:
    def __init__(self, nf, me, piece, recv, up, down, across):
        self.nl = nf // 2
        self.me, self.z, self.x = me, me // 2, me % 2
        self.piece, self.recv = piece, recv
        self.sems = {"up": up, "down": down, "across": across}

    def copy(self, slot, way):
        target = {"up": self.me + 2, "down": self.me - 2, "across": self.me + 1 - 2 * self.x}[way]
        return remote(self.piece(slot), self.piece(slot), self.sems[way].at[slot], self.recv.at[slot], fs=target)

    def arrive(self, slot):
        self.copy(slot, "across").wait_recv()

    def open(self):
        @pl.when(self.z < self.nl - 1)
        def _():
            self.copy(self.me, "up").start()

        @pl.when(self.z > 0)
        def _():
            self.copy(self.me, "down").start()

        self.copy(self.me, "across").start()

    def step(self, dist, then=lambda slot: None):
        @pl.when(self.z >= dist)
        def _():
            slot = self.me - 2 * dist
            self.arrive(slot)

            @pl.when(self.z < self.nl - 1)
            def _():
                self.copy(slot, "up").start()

            self.copy(slot, "across").start()
            then(slot)

        @pl.when(self.z + dist < self.nl)
        def _():
            slot = self.me + 2 * dist
            self.arrive(slot)

            @pl.when(self.z > 0)
            def _():
                self.copy(slot, "down").start()

            self.copy(slot, "across").start()
            then(slot)

    def other(self, dist, then=lambda slot: None):
        pair = self.me + 1 - 2 * self.x
        if dist == 0:
            self.arrive(pair)
            then(pair)
            return

        @pl.when(self.z >= dist)
        def _():
            self.arrive(pair - 2 * dist)
            then(pair - 2 * dist)

        @pl.when(self.z + dist < self.nl)
        def _():
            self.arrive(pair + 2 * dist)
            then(pair + 2 * dist)

    def close(self):
        for line in range(self.nl):
            slot = 2 * line + self.x

            @pl.when((self.z >= line) & (self.z < self.nl - 1))
            def _():
                self.copy(slot, "up").wait_send()

            @pl.when((self.z <= line) & (self.z > 0))
            def _():
                self.copy(slot, "down").wait_send()

            self.copy(slot, "across").wait_send()


def main_kernel(nf, nt, *refs):
    x_in, c_in, f_in, w_in = refs[0], refs[1:3], refs[3:5], refs[5:7]
    first_in, second_in = refs[7:9], refs[9:11]
    step_out, new_out, copy_out, first_out, second_out = (refs[i : i + 2] for i in range(11, 21, 2))
    (xv, cv, fbuf, rl, rs, rfull, ss, wv, m1, m2, stv, nwv, fnv, snv, cbuf) = refs[21:36]
    (in_sem, out_sem, f_sem, core_sem, rs_sem, ag_sem, ss_sem, cp_sem, co_sem) = refs[36:]
    me, tp = lax.axis_index("fs"), lax.axis_index("tp")
    depth = f_in[0].shape[0]
    rank = f_in[0].shape[1]
    half = depth // 2
    core = tp % 2
    mate = tp + 1 - 2 * core
    pr = rs.shape[1]

    def block(slot):
        return pl.ds(pl.multiple_of(slot * depth, depth), depth)

    loads = [pltpu.make_async_copy(f_in[p], fbuf.at[block(me), pl.ds(p * rank, rank)], in_sem.at[p]) for p in range(2)]
    loads += [pltpu.make_async_copy(x_in, xv, in_sem.at[2])]
    for i, (src, dst) in enumerate(((c_in, cv), (first_in, m1), (second_in, m2), (w_in, wv))):
        loads += [pltpu.make_async_copy(src[p], dst.at[p], in_sem.at[3 + 2 * i + p]) for p in range(2)]
    for load in loads:
        load.start()

    barrier = pltpu.get_barrier_semaphore()
    for k in range(1, nf):
        pl.semaphore_signal(barrier, inc=1, device_id={"fs": (me + k) % nf}, device_id_type=pl.DeviceIdType.MESH)
    for k in range(1, nt):
        pl.semaphore_signal(barrier, inc=1, device_id={"tp": (tp + k) % nt}, device_id_type=pl.DeviceIdType.MESH)
    pl.semaphore_wait(barrier, nf + nt - 2)

    def half_of(slot, which):
        return fbuf.at[pl.ds(pl.multiple_of(slot * depth + which * half, half), half), :]

    gather = Line(nf, me, lambda slot: half_of(slot, core), f_sem.at[0], f_sem.at[1], f_sem.at[2], f_sem.at[3])

    def hand(slot):
        view = half_of(slot, core)
        return remote(view, view, core_sem.at[0, slot], core_sem.at[1, slot], tp=mate)

    def take(slot):
        view = half_of(slot, 1 - core)
        remote(view, view, core_sem.at[0, slot], core_sem.at[1, slot], tp=mate).wait_recv()

    loads[0].wait()
    loads[1].wait()
    gather.open()
    pass_on = lambda slot: hand(slot).start()
    gather.other(0, pass_on)
    for dist in range(1, nf // 2):
        gather.step(dist, pass_on)
        gather.other(dist, pass_on)
    for load in loads[2:5]:
        load.wait()
    for k in range(1, nf):
        take((me + k) % nf)

    rows = jnp.dot(xv[...], fbuf[...], preferred_element_type=F32)
    terms = parts(rows, 2)
    for p in range(2):
        total = 0.0
        for term in terms:
            total = total + lax.dot_general(
                term[:, p * rank : (p + 1) * rank], cv[p], (((0,), (0,)), ((), ())), preferred_element_type=F32
            )
        rl[p * rank : (p + 1) * rank, :] = total

    def piece(slot):
        return pl.ds(pl.multiple_of(slot * pr, pr), pr)

    def scatter(k):
        to = (me + k) % nf
        return remote(rl.at[piece(to), :], rs.at[me], rs_sem.at[0, k], rs_sem.at[1, me], fs=to)

    for k in range(1, nf):
        scatter(k).start()
    summed = rl[piece(me), :]
    for k in range(1, nf):
        frm = (me + k) % nf
        remote(rl.at[piece(me), :], rs.at[frm], rs_sem.at[0, k], rs_sem.at[1, frm], fs=frm).wait_recv()
        summed = summed + rs[frm]
    rfull[piece(me), :] = summed

    def spread(k):
        view = rfull.at[piece(me), :]
        return remote(view, view, ag_sem.at[0, k], ag_sem.at[1, me], fs=(me + k) % nf)

    for k in range(1, nf):
        spread(k).start()
    for load in loads[5:]:
        load.wait()
    for k in range(1, nf):
        frm = (me + k) % nf
        view = rfull.at[piece(frm), :]
        remote(view, view, ag_sem.at[0, k], ag_sem.at[1, frm], fs=frm).wait_recv()

    squares = jnp.zeros((), F32)
    directions = []
    for p in range(2):
        projected = rfull[p * rank : (p + 1) * rank, :]
        first_new, second_new, direction = update_moments(projected, m1[p], m2[p])
        fnv[p] = first_new
        snv[p] = second_new
        squares = squares + jnp.sum(direction * direction)
        directions.append(direction)
    ss[tp] = jnp.full(ss.shape[1:], squares, F32)

    def tell(k):
        return remote(ss.at[tp], ss.at[tp], ss_sem.at[0, k], ss_sem.at[1, tp], tp=(tp + k) % nt)

    for k in range(1, nt):
        tell(k).start()
    raw = []
    for p in range(2):
        own = fbuf[block(me), p * rank : (p + 1) * rank]
        total = 0.0
        for term in reversed(parts(directions[p], 3)):
            total = total + jnp.dot(own, term, preferred_element_type=F32)
        raw.append(total)
    for k in range(1, nt):
        frm = (tp + k) % nt
        remote(ss.at[frm], ss.at[frm], ss_sem.at[0, k], ss_sem.at[1, frm], tp=frm).wait_recv()
    total = ss[0]
    for t in range(1, nt):
        total = total + ss[t]
    entries = 2 * rank * directions[0].shape[1] * nt
    scale = (learn_rate / jnp.sqrt(total / entries + 1e-06))[0:1, 0:1]

    lines = []
    for p in range(2):
        step = -scale * raw[p]
        stv[p] = step
        new = wv[p] + step
        nwv[p] = new
        cbuf[p, block(me), :] = new.astype(BF)
        lines.append(
            Line(
                nf,
                me,
                functools.partial(lambda p, slot: cbuf.at[p, block(slot), :], p),
                cp_sem.at[p, 0],
                cp_sem.at[p, 1],
                cp_sem.at[p, 2],
                cp_sem.at[p, 3],
            )
        )
        lines[p].open()
    outs = []
    for i, (src, dst) in enumerate(((fnv, first_out), (snv, second_out), (stv, step_out), (nwv, new_out))):
        outs += [pltpu.make_async_copy(src.at[p], dst[p], out_sem.at[2 * i + p]) for p in range(2)]
    for out in outs:
        out.start()

    def put(p, slot):
        return pltpu.make_async_copy(cbuf.at[p, block(slot), :], copy_out[p].at[block(slot), :], co_sem.at[p, slot])

    starts = [functools.partial(lambda p, slot: put(p, slot).start(), p) for p in range(2)]
    for p in range(2):
        starts[p](me)
    for dist in range(1, nf // 2):
        for p in range(2):
            lines[p].step(dist, starts[p])
        for p in range(2):
            lines[p].other(dist - 1, starts[p])
    for p in range(2):
        lines[p].other(nf // 2 - 1, starts[p])

    gather.close()
    for line in lines:
        line.close()
    for k in range(1, nf):
        hand((me + k) % nf).wait_send()
        scatter(k).wait_send()
        spread(k).wait_send()
    for k in range(1, nt):
        tell(k).wait_send()
    for out in outs:
        out.wait()
    for p in range(2):
        for slot in range(nf):
            put(p, slot).wait()


def out_kernel(n, *refs):
    copies = [pltpu.make_async_copy(refs[i], refs[n + i], refs[2 * n].at[i]) for i in range(n)]
    for copy in copies:
        copy.start()
    for copy in copies:
        copy.wait()


def fused(nf, nt, *args):
    x, cot, factor, weight, first = args[0], args[1], args[3], args[5], args[7]
    tokens, width = cot.shape
    depth, rank = factor.shape
    pr = 2 * rank // nf
    shape = jax.ShapeDtypeStruct
    outs = [shape(weight.shape, F32)] * 4 + [shape((nf * depth, width), BF)] * 2 + [shape(first.shape, F32)] * 4
    anywhere, hbm = pl.BlockSpec(memory_space=pl.ANY), pl.BlockSpec(memory_space=pltpu.HBM)
    vmem, dma = pltpu.VMEM, pltpu.SemaphoreType.DMA
    results = pl.pallas_call(
        functools.partial(main_kernel, nf, nt),
        out_shape=outs,
        in_specs=[hbm] * 11,
        out_specs=[anywhere] * 10,
        scratch_shapes=[
            vmem(x.shape, BF),
            vmem((2, tokens, width), BF),
            vmem((nf * depth, 2 * rank), BF),
            vmem((2 * rank, width), F32),
            vmem((nf, pr, width), F32),
            vmem((2 * rank, width), F32),
            vmem((nt, 8, 128), F32),
            vmem((2, depth, width), F32),
            vmem((2, rank, width), F32),
            vmem((2, rank, width), F32),
            vmem((2, depth, width), F32),
            vmem((2, depth, width), F32),
            vmem((2, rank, width), F32),
            vmem((2, rank, width), F32),
            vmem((2, nf * depth, width), BF),
            dma((11,)),
            dma((8,)),
            dma((4, nf)),
            dma((2, nf)),
            dma((2, nf)),
            dma((2, nf)),
            dma((2, nt)),
            dma((2, 4, nf)),
            dma((2, nf)),
        ],
        compiler_params=pltpu.CompilerParams(
            collective_id=0, has_side_effects=True, vmem_limit_bytes=24 * 1024 * 1024
        ),
    )(*[pltpu.with_memory_space_constraint(a, pltpu.HBM) for a in args])
    return pl.pallas_call(
        functools.partial(out_kernel, len(outs)),
        out_shape=outs,
        in_specs=[anywhere] * 10,
        out_specs=[hbm] * 10,
        scratch_shapes=[dma((len(outs),))],
        compiler_params=pltpu.CompilerParams(vmem_limit_bytes=1024 * 1024),
    )(*results)


def fits(nf, nt, depth, rank):
    return nf % 2 == 0 and nt % 2 == 0 and nf <= 16 and depth % 32 == 0 and (2 * rank) % (8 * nf) == 0


def device_step(nf, nt, *args):
    depth, rank = args[3].shape
    if fits(nf, nt, depth, rank):
        return tuple(fused(nf, nt, *args))
    return local(*args)


def solution(mesh):
    return jax.shard_map(
        functools.partial(device_step, mesh.shape["fs"], mesh.shape["tp"]),
        mesh=mesh,
        in_specs=(
            P("fs", None),
            P("fs", "tp"),
            P("fs", "tp"),
            P("fs", None),
            P("fs", None),
            P("fs", "tp"),
            P("fs", "tp"),
            P(None, "tp"),
            P(None, "tp"),
            P(None, "tp"),
            P(None, "tp"),
        ),
        out_specs=(
            P("fs", "tp"),
            P("fs", "tp"),
            P("fs", "tp"),
            P("fs", "tp"),
            P(None, "tp"),
            P(None, "tp"),
            P(None, "tp"),
            P(None, "tp"),
            P(None, "tp"),
            P(None, "tp"),
        ),
        check_vma=False,
    )
```

```python
import functools

import jax
import jax.numpy as jnp
from jax import lax
from jax.experimental import pallas as pl
from jax.experimental.pallas import tpu as pltpu
from jax.sharding import PartitionSpec as P

first_decay = 0.8
second_decay = 0.9
learn_rate = 0.5


def update_moments(projected, first_old, second_old):
    first_new = first_decay * first_old + (1.0 - first_decay) * projected
    second_new = second_decay * second_old + (1.0 - second_decay) * projected * projected
    return (first_new, second_new, first_new / jnp.sqrt(second_new))


def local(
    layer_input,
    branch_cotangent,
    gate_cotangent,
    branch_factor,
    gate_factor,
    branch_weight,
    gate_weight,
    branch_first,
    gate_first,
    branch_second,
    gate_second,
):
    highest = lax.Precision.HIGHEST
    width = branch_cotangent.shape[1]
    branch_whole, gate_whole = (
        lax.all_gather(branch_factor, "fs", axis=0, tiled=True),
        lax.all_gather(gate_factor, "fs", axis=0, tiled=True),
    )
    branch_rows = jnp.dot(layer_input, branch_whole, preferred_element_type=jnp.float32)
    gate_rows = jnp.dot(layer_input, gate_whole, preferred_element_type=jnp.float32)
    branch_local = jnp.einsum(
        "tr,tw->rw", branch_rows, branch_cotangent.astype(jnp.float32), precision=highest
    )
    gate_local = jnp.einsum(
        "tr,tw->rw", gate_rows, gate_cotangent.astype(jnp.float32), precision=highest
    )
    branch_projected, gate_projected = lax.psum((branch_local, gate_local), "fs")
    branch_first_new, branch_second_new, branch_direction = update_moments(
        branch_projected, branch_first, branch_second
    )
    gate_first_new, gate_second_new, gate_direction = update_moments(
        gate_projected, gate_first, gate_second
    )
    local_squares = jnp.sum(branch_direction * branch_direction) + jnp.sum(
        gate_direction * gate_direction
    )
    sum_squares = lax.psum(local_squares, "tp")
    entries = 2 * branch_direction.shape[0] * width * lax.axis_size("tp")
    step_scale = learn_rate / jnp.sqrt(sum_squares / entries + 1e-06)
    branch_step = -step_scale * jnp.dot(
        branch_factor.astype(jnp.float32), branch_direction, precision=highest
    )
    gate_step = -step_scale * jnp.dot(
        gate_factor.astype(jnp.float32), gate_direction, precision=highest
    )
    branch_new = branch_weight + branch_step
    gate_new = gate_weight + gate_step
    branch_copy, gate_copy = (
        lax.all_gather(branch_new.astype(jnp.bfloat16), "fs", axis=0, tiled=True),
        lax.all_gather(gate_new.astype(jnp.bfloat16), "fs", axis=0, tiled=True),
    )
    return (
        branch_step,
        gate_step,
        branch_new,
        gate_new,
        branch_copy,
        gate_copy,
        branch_first_new,
        gate_first_new,
        branch_second_new,
        gate_second_new,
    )


BF, F32 = jnp.bfloat16, jnp.float32
SPLIT = 2


def parts(value, count):
    terms = []
    for _ in range(count):
        term = value.astype(BF)
        terms.append(term)
        value = value - term.astype(F32)
    return terms


def remote(src, dst, send_sem, recv_sem, **where):
    return pltpu.make_async_remote_copy(
        src_ref=src,
        dst_ref=dst,
        send_sem=send_sem,
        recv_sem=recv_sem,
        device_id=where,
        device_id_type=pl.DeviceIdType.MESH,
    )


class Line:
    def __init__(self, nf, me, own, piece, recv, up, down, across, shift=False):
        self.nl = nf // 2
        self.own, self.shift = own, shift
        self.me, self.z, self.x = me, me // 2, me % 2
        self.piece, self.recv = piece, recv
        self.sems = {"up": up, "down": down, "across": across}

    def copy(self, slot, way):
        target = {"up": self.me + 2, "down": self.me - 2, "across": self.me + 1 - 2 * self.x}[way]
        src = self.own if slot is self.me else self.piece(slot)
        return remote(src, self.piece(slot), self.sems[way].at[slot], self.recv.at[slot], fs=target)

    def arrive(self, slot):
        self.copy(slot, "across").wait_recv()

    def both(self, slot, act):
        @pl.when(self.z < self.nl - 1)
        def _():
            act(self.copy(slot, "up"))

        @pl.when(self.z > 0)
        def _():
            act(self.copy(slot, "down"))

    def open(self):
        self.copy(self.me, "across").start()
        self.both(self.me, lambda copy: copy.start())

    def step(self, dist, then=lambda slot: None):
        @pl.when(self.z >= dist)
        def _():
            slot = self.me - 2 * dist
            self.arrive(slot)

            @pl.when(self.z < self.nl - 1)
            def _():
                self.copy(slot, "up").start()

            if not (self.shift and dist == 1):
                self.copy(slot, "across").start()
            then(slot)

        @pl.when(self.z + dist < self.nl)
        def _():
            slot = self.me + 2 * dist
            self.arrive(slot)

            @pl.when(self.z > 0)
            def _():
                self.copy(slot, "down").start()

            if not (self.shift and dist == 1):
                self.copy(slot, "across").start()
            then(slot)

    def other(self, dist, then=lambda slot: None):
        pair = self.me + 1 - 2 * self.x
        if dist == 0:
            self.arrive(pair)
            if self.shift:
                self.both(pair, lambda copy: copy.start())
            then(pair)
            return

        @pl.when(self.z >= dist)
        def _():
            self.arrive(pair - 2 * dist)
            then(pair - 2 * dist)

        @pl.when(self.z + dist < self.nl)
        def _():
            self.arrive(pair + 2 * dist)
            then(pair + 2 * dist)

    def close(self):
        for line in range(self.nl):
            slot = 2 * line + self.x

            @pl.when((self.z >= line) & (self.z < self.nl - 1))
            def _():
                self.copy(slot, "up").wait_send()

            @pl.when((self.z <= line) & (self.z > 0))
            def _():
                self.copy(slot, "down").wait_send()

            if self.shift:

                @pl.when((self.z != line - 1) & (self.z != line + 1))
                def _():
                    self.copy(slot, "across").wait_send()

            else:
                self.copy(slot, "across").wait_send()

        if self.shift:
            self.both(self.me + 1 - 2 * self.x, lambda copy: copy.wait_send())


def main_kernel(nf, nt, *refs):
    x_in, c_in, f_in, w_in = refs[0], refs[1:3], refs[3:5], refs[5:7]
    first_in, second_in = refs[7:9], refs[9:11]
    step_out, new_out, copy_out, first_out, second_out = (refs[i : i + 2] for i in range(11, 21, 2))
    (xv, cv, fbuf, rl, rs, rfull, ss, wv, m1, m2, stv, nwv, fnv, snv, cbuf) = refs[21:36]
    (in_sem, out_sem, f_sem, core_sem, rs_sem, ag_sem, ss_sem, cp_sem) = refs[36:]
    me, tp = lax.axis_index("fs"), lax.axis_index("tp")
    depth = f_in[0].shape[0]
    rank = f_in[0].shape[1]
    half = depth // 2
    core = tp % 2
    mate = tp + 1 - 2 * core
    pr = rs.shape[1]

    def block(slot):
        return pl.ds(pl.multiple_of(slot * depth, depth), depth)

    loads = [pltpu.make_async_copy(f_in[p], fbuf.at[block(me), pl.ds(p * rank, rank)], in_sem.at[p]) for p in range(2)]
    loads += [pltpu.make_async_copy(x_in, xv, in_sem.at[2])]
    for i, (src, dst) in enumerate(((c_in, cv), (first_in, m1), (second_in, m2), (w_in, wv))):
        loads += [pltpu.make_async_copy(src[p], dst.at[p], in_sem.at[3 + 2 * i + p]) for p in range(2)]
    for load in loads:
        load.start()

    barrier = pltpu.get_barrier_semaphore()
    for k in range(1, nf):
        pl.semaphore_signal(barrier, inc=1, device_id={"fs": (me + k) % nf}, device_id_type=pl.DeviceIdType.MESH)
    for k in range(1, nt):
        pl.semaphore_signal(barrier, inc=1, device_id={"tp": (tp + k) % nt}, device_id_type=pl.DeviceIdType.MESH)
    pl.semaphore_wait(barrier, nf + nt - 2)

    def half_of(slot, which):
        return fbuf.at[pl.ds(pl.multiple_of(slot * depth + which * half, half), half), :]

    gather = Line(nf, me, half_of(me, core), lambda slot: half_of(slot, core), f_sem.at[0], f_sem.at[1], f_sem.at[2], f_sem.at[3])

    def hand(slot):
        view = half_of(slot, core)
        return remote(view, view, core_sem.at[0, slot], core_sem.at[1, slot], tp=mate)

    def take(slot):
        view = half_of(slot, 1 - core)
        remote(view, view, core_sem.at[0, slot], core_sem.at[1, slot], tp=mate).wait_recv()

    loads[0].wait()
    loads[1].wait()
    gather.open()
    pass_on = lambda slot: hand(slot).start()
    gather.other(0, pass_on)
    for dist in range(1, nf // 2):
        gather.step(dist, pass_on)
        gather.other(dist, pass_on)
    for load in loads[2:5]:
        load.wait()
    for k in range(1, nf):
        take((me + k) % nf)

    rows = jnp.dot(xv[...], fbuf[...], preferred_element_type=F32)
    terms = parts(rows, 2)
    for p in range(2):
        total = 0.0
        for term in terms:
            total = total + lax.dot_general(
                term[:, p * rank : (p + 1) * rank], cv[p], (((0,), (0,)), ((), ())), preferred_element_type=F32
            )
        rl[p * rank : (p + 1) * rank, :] = total

    def piece(slot):
        return pl.ds(pl.multiple_of(slot * pr, pr), pr)

    def scatter(k):
        to = (me + k) % nf
        return remote(rl.at[piece(to), :], rs.at[me], rs_sem.at[0, k], rs_sem.at[1, me], fs=to)

    for k in range(1, nf):
        scatter(k).start()
    summed = rl[piece(me), :]
    for k in range(1, nf):
        frm = (me + k) % nf
        remote(rl.at[piece(me), :], rs.at[frm], rs_sem.at[0, k], rs_sem.at[1, frm], fs=frm).wait_recv()
        summed = summed + rs[frm]
    rfull[piece(me), :] = summed

    def spread(k):
        view = rfull.at[piece(me), :]
        return remote(view, view, ag_sem.at[0, k], ag_sem.at[1, me], fs=(me + k) % nf)

    for k in range(1, nf):
        spread(k).start()
    for load in loads[5:]:
        load.wait()
    for k in range(1, nf):
        frm = (me + k) % nf
        view = rfull.at[piece(frm), :]
        remote(view, view, ag_sem.at[0, k], ag_sem.at[1, frm], fs=frm).wait_recv()

    squares = jnp.zeros((), F32)
    directions = []
    for p in range(2):
        projected = rfull[p * rank : (p + 1) * rank, :]
        first_new, second_new, direction = update_moments(projected, m1[p], m2[p])
        fnv[p] = first_new
        snv[p] = second_new
        squares = squares + jnp.sum(direction * direction)
        directions.append(direction)
    ss[tp] = jnp.full(ss.shape[1:], squares, F32)

    def tell(k):
        return remote(ss.at[tp], ss.at[tp], ss_sem.at[0, k], ss_sem.at[1, tp], tp=(tp + k) % nt)

    for k in range(1, nt):
        tell(k).start()
    raw = []
    for p in range(2):
        own = fbuf[block(me), p * rank : (p + 1) * rank]
        total = 0.0
        for term in reversed(parts(directions[p], 3)):
            total = total + jnp.dot(own, term, preferred_element_type=F32)
        raw.append(total)
    for k in range(1, nt):
        frm = (tp + k) % nt
        remote(ss.at[frm], ss.at[frm], ss_sem.at[0, k], ss_sem.at[1, frm], tp=frm).wait_recv()
    total = ss[0]
    for t in range(1, nt):
        total = total + ss[t]
    entries = 2 * rank * directions[0].shape[1] * nt
    scale = (learn_rate / jnp.sqrt(total / entries + 1e-06))[0:1, 0:1]

    cut = depth // SPLIT

    def rows_of(slot, part):
        return pl.ds(pl.multiple_of(slot * depth + part * cut, cut), cut)

    lines = []
    for p in range(2):
        step = -scale * raw[p]
        new = wv[p] + step
        cbuf[p] = new.astype(BF)
        stv[p] = step
        nwv[p] = new
        for part in range(SPLIT):
            i = p * SPLIT + part
            own = cbuf.at[p, part * cut : (part + 1) * cut, :]
            piece_of = functools.partial(lambda p, part, slot: copy_out[p].at[rows_of(slot, part), :], p, part)
            lines.append(Line(nf, me, own, piece_of, *(cp_sem.at[i, j] for j in range(4)), shift=p == 1))
            lines[i].open()
    outs = []
    for i, (src, dst) in enumerate(((fnv, first_out), (snv, second_out), (stv, step_out), (nwv, new_out))):
        outs += [pltpu.make_async_copy(src.at[p], dst[p], out_sem.at[2 * i + p]) for p in range(2)]
    for p in range(2):
        outs += [pltpu.make_async_copy(cbuf.at[p], copy_out[p].at[block(me), :], out_sem.at[8 + p])]
    for out in outs:
        out.start()
    for dist in range(1, nf // 2):
        for line in lines:
            line.step(dist)
        if dist == 1:
            for line in lines:
                line.other(0)
    for dist in range(1, nf // 2):
        for line in lines:
            line.other(dist)

    gather.close()
    for line in lines:
        line.close()
    for k in range(1, nf):
        hand((me + k) % nf).wait_send()
        scatter(k).wait_send()
        spread(k).wait_send()
    for k in range(1, nt):
        tell(k).wait_send()
    for out in outs:
        out.wait()


def out_kernel(n, *refs):
    copies = [pltpu.make_async_copy(refs[i], refs[n + i], refs[2 * n].at[i]) for i in range(n)]
    for copy in copies:
        copy.start()
    for copy in copies:
        copy.wait()


def fused(nf, nt, *args):
    x, cot, factor, weight, first = args[0], args[1], args[3], args[5], args[7]
    tokens, width = cot.shape
    depth, rank = factor.shape
    pr = 2 * rank // nf
    shape = jax.ShapeDtypeStruct
    outs = [shape(weight.shape, F32)] * 4 + [shape((nf * depth, width), BF)] * 2 + [shape(first.shape, F32)] * 4
    anywhere, hbm = pl.BlockSpec(memory_space=pl.ANY), pl.BlockSpec(memory_space=pltpu.HBM)
    vmem, dma = pltpu.VMEM, pltpu.SemaphoreType.DMA
    results = pl.pallas_call(
        functools.partial(main_kernel, nf, nt),
        out_shape=outs,
        in_specs=[hbm] * 11,
        out_specs=[anywhere] * 10,
        scratch_shapes=[
            vmem(x.shape, BF),
            vmem((2, tokens, width), BF),
            vmem((nf * depth, 2 * rank), BF),
            vmem((2 * rank, width), F32),
            vmem((nf, pr, width), F32),
            vmem((2 * rank, width), F32),
            vmem((nt, 8, 128), F32),
            vmem((2, depth, width), F32),
            vmem((2, rank, width), F32),
            vmem((2, rank, width), F32),
            vmem((2, depth, width), F32),
            vmem((2, depth, width), F32),
            vmem((2, rank, width), F32),
            vmem((2, rank, width), F32),
            vmem((2, depth, width), BF),
            dma((11,)),
            dma((10,)),
            dma((4, nf)),
            dma((2, nf)),
            dma((2, nf)),
            dma((2, nf)),
            dma((2, nt)),
            dma((2 * SPLIT, 4, nf)),
        ],
        compiler_params=pltpu.CompilerParams(
            collective_id=0, has_side_effects=True, vmem_limit_bytes=24 * 1024 * 1024
        ),
    )(*[pltpu.with_memory_space_constraint(a, pltpu.HBM) for a in args])
    return pl.pallas_call(
        functools.partial(out_kernel, len(outs)),
        out_shape=outs,
        in_specs=[anywhere] * 10,
        out_specs=[hbm] * 10,
        scratch_shapes=[dma((len(outs),))],
        compiler_params=pltpu.CompilerParams(vmem_limit_bytes=1024 * 1024),
    )(*results)


def fits(nf, nt, depth, rank):
    return nf % 2 == 0 and nt % 2 == 0 and nf <= 16 and depth % (16 * SPLIT) == 0 and (2 * rank) % (8 * nf) == 0


def device_step(nf, nt, *args):
    depth, rank = args[3].shape
    if fits(nf, nt, depth, rank):
        return tuple(fused(nf, nt, *args))
    return local(*args)


def solution(mesh):
    return jax.shard_map(
        functools.partial(device_step, mesh.shape["fs"], mesh.shape["tp"]),
        mesh=mesh,
        in_specs=(
            P("fs", None),
            P("fs", "tp"),
            P("fs", "tp"),
            P("fs", None),
            P("fs", None),
            P("fs", "tp"),
            P("fs", "tp"),
            P(None, "tp"),
            P(None, "tp"),
            P(None, "tp"),
            P(None, "tp"),
        ),
        out_specs=(
            P("fs", "tp"),
            P("fs", "tp"),
            P("fs", "tp"),
            P("fs", "tp"),
            P(None, "tp"),
            P(None, "tp"),
            P(None, "tp"),
            P(None, "tp"),
            P(None, "tp"),
            P(None, "tp"),
        ),
        check_vma=False,
    )
```

```python
import functools

import jax
import jax.numpy as jnp
from jax import lax
from jax.experimental import pallas as pl
from jax.experimental.pallas import tpu as pltpu
from jax.sharding import PartitionSpec as P

first_decay = 0.8
second_decay = 0.9
learn_rate = 0.5


def update_moments(projected, first_old, second_old):
    first_new = first_decay * first_old + (1.0 - first_decay) * projected
    second_new = second_decay * second_old + (1.0 - second_decay) * projected * projected
    return (first_new, second_new, first_new / jnp.sqrt(second_new))


def local(
    layer_input,
    branch_cotangent,
    gate_cotangent,
    branch_factor,
    gate_factor,
    branch_weight,
    gate_weight,
    branch_first,
    gate_first,
    branch_second,
    gate_second,
):
    highest = lax.Precision.HIGHEST
    width = branch_cotangent.shape[1]
    branch_whole, gate_whole = (
        lax.all_gather(branch_factor, "fs", axis=0, tiled=True),
        lax.all_gather(gate_factor, "fs", axis=0, tiled=True),
    )
    branch_rows = jnp.dot(layer_input, branch_whole, preferred_element_type=jnp.float32)
    gate_rows = jnp.dot(layer_input, gate_whole, preferred_element_type=jnp.float32)
    branch_local = jnp.einsum(
        "tr,tw->rw", branch_rows, branch_cotangent.astype(jnp.float32), precision=highest
    )
    gate_local = jnp.einsum(
        "tr,tw->rw", gate_rows, gate_cotangent.astype(jnp.float32), precision=highest
    )
    branch_projected, gate_projected = lax.psum((branch_local, gate_local), "fs")
    branch_first_new, branch_second_new, branch_direction = update_moments(
        branch_projected, branch_first, branch_second
    )
    gate_first_new, gate_second_new, gate_direction = update_moments(
        gate_projected, gate_first, gate_second
    )
    local_squares = jnp.sum(branch_direction * branch_direction) + jnp.sum(
        gate_direction * gate_direction
    )
    sum_squares = lax.psum(local_squares, "tp")
    entries = 2 * branch_direction.shape[0] * width * lax.axis_size("tp")
    step_scale = learn_rate / jnp.sqrt(sum_squares / entries + 1e-06)
    branch_step = -step_scale * jnp.dot(
        branch_factor.astype(jnp.float32), branch_direction, precision=highest
    )
    gate_step = -step_scale * jnp.dot(
        gate_factor.astype(jnp.float32), gate_direction, precision=highest
    )
    branch_new = branch_weight + branch_step
    gate_new = gate_weight + gate_step
    branch_copy, gate_copy = (
        lax.all_gather(branch_new.astype(jnp.bfloat16), "fs", axis=0, tiled=True),
        lax.all_gather(gate_new.astype(jnp.bfloat16), "fs", axis=0, tiled=True),
    )
    return (
        branch_step,
        gate_step,
        branch_new,
        gate_new,
        branch_copy,
        gate_copy,
        branch_first_new,
        gate_first_new,
        branch_second_new,
        gate_second_new,
    )


BF, F32 = jnp.bfloat16, jnp.float32
SPLIT = 4


def parts(value, count):
    terms = []
    for _ in range(count):
        term = value.astype(BF)
        terms.append(term)
        value = value - term.astype(F32)
    return terms


def remote(src, dst, send_sem, recv_sem, **where):
    return pltpu.make_async_remote_copy(
        src_ref=src,
        dst_ref=dst,
        send_sem=send_sem,
        recv_sem=recv_sem,
        device_id=where,
        device_id_type=pl.DeviceIdType.MESH,
    )


class Line:
    def __init__(self, nf, me, own, piece, recv, up, down, across, shift=False):
        self.nl = nf // 2
        self.own, self.shift = own, shift
        self.me, self.z, self.x = me, me // 2, me % 2
        self.piece, self.recv = piece, recv
        self.sems = {"up": up, "down": down, "across": across}

    def copy(self, slot, way):
        target = {"up": self.me + 2, "down": self.me - 2, "across": self.me + 1 - 2 * self.x}[way]
        src = self.own if slot is self.me else self.piece(slot)
        return remote(src, self.piece(slot), self.sems[way].at[slot], self.recv.at[slot], fs=target)

    def arrive(self, slot):
        self.copy(slot, "across").wait_recv()

    def both(self, slot, act):
        @pl.when(self.z < self.nl - 1)
        def _():
            act(self.copy(slot, "up"))

        @pl.when(self.z > 0)
        def _():
            act(self.copy(slot, "down"))

    def open(self):
        self.copy(self.me, "across").start()
        self.both(self.me, lambda copy: copy.start())

    def step(self, dist, then=lambda slot: None):
        @pl.when(self.z >= dist)
        def _():
            slot = self.me - 2 * dist
            self.arrive(slot)

            @pl.when(self.z < self.nl - 1)
            def _():
                self.copy(slot, "up").start()

            if not (self.shift and dist == 1):
                self.copy(slot, "across").start()
            then(slot)

        @pl.when(self.z + dist < self.nl)
        def _():
            slot = self.me + 2 * dist
            self.arrive(slot)

            @pl.when(self.z > 0)
            def _():
                self.copy(slot, "down").start()

            if not (self.shift and dist == 1):
                self.copy(slot, "across").start()
            then(slot)

    def other(self, dist, then=lambda slot: None):
        pair = self.me + 1 - 2 * self.x
        if dist == 0:
            self.arrive(pair)
            if self.shift:
                self.both(pair, lambda copy: copy.start())
            then(pair)
            return

        @pl.when(self.z >= dist)
        def _():
            self.arrive(pair - 2 * dist)
            then(pair - 2 * dist)

        @pl.when(self.z + dist < self.nl)
        def _():
            self.arrive(pair + 2 * dist)
            then(pair + 2 * dist)

    def close(self):
        for line in range(self.nl):
            slot = 2 * line + self.x

            @pl.when((self.z >= line) & (self.z < self.nl - 1))
            def _():
                self.copy(slot, "up").wait_send()

            @pl.when((self.z <= line) & (self.z > 0))
            def _():
                self.copy(slot, "down").wait_send()

            if self.shift:

                @pl.when((self.z != line - 1) & (self.z != line + 1))
                def _():
                    self.copy(slot, "across").wait_send()

            else:
                self.copy(slot, "across").wait_send()

        if self.shift:
            self.both(self.me + 1 - 2 * self.x, lambda copy: copy.wait_send())


def main_kernel(nf, nt, *refs):
    x_in, c_in, f_in, w_in = refs[0], refs[1:3], refs[3:5], refs[5:7]
    first_in, second_in = refs[7:9], refs[9:11]
    step_out, new_out, copy_out, first_out, second_out = (refs[i : i + 2] for i in range(11, 21, 2))
    (xv, cv, fbuf, rl, rs, rfull, ss, wv, m1, m2, stv, nwv, fnv, snv, cbuf) = refs[21:36]
    (in_sem, out_sem, f_sem, core_sem, rs_sem, ag_sem, ss_sem, cp_sem) = refs[36:]
    me, tp = lax.axis_index("fs"), lax.axis_index("tp")
    depth = f_in[0].shape[0]
    rank = f_in[0].shape[1]
    half = depth // 2
    core = tp % 2
    mate = tp + 1 - 2 * core
    pr = rs.shape[1]

    def block(slot):
        return pl.ds(pl.multiple_of(slot * depth, depth), depth)

    loads = [pltpu.make_async_copy(f_in[p], fbuf.at[block(me), pl.ds(p * rank, rank)], in_sem.at[p]) for p in range(2)]
    loads += [pltpu.make_async_copy(x_in, xv, in_sem.at[2])]
    for i, (src, dst) in enumerate(((c_in, cv), (first_in, m1), (second_in, m2), (w_in, wv))):
        loads += [pltpu.make_async_copy(src[p], dst.at[p], in_sem.at[3 + 2 * i + p]) for p in range(2)]
    for load in loads:
        load.start()

    barrier = pltpu.get_barrier_semaphore()
    for k in range(1, nf):
        pl.semaphore_signal(barrier, inc=1, device_id={"fs": (me + k) % nf}, device_id_type=pl.DeviceIdType.MESH)
    for k in range(1, nt):
        pl.semaphore_signal(barrier, inc=1, device_id={"tp": (tp + k) % nt}, device_id_type=pl.DeviceIdType.MESH)
    pl.semaphore_wait(barrier, nf + nt - 2)

    def half_of(slot, which):
        return fbuf.at[pl.ds(pl.multiple_of(slot * depth + which * half, half), half), :]

    gather = Line(nf, me, half_of(me, core), lambda slot: half_of(slot, core), f_sem.at[0], f_sem.at[1], f_sem.at[2], f_sem.at[3])

    def hand(slot):
        view = half_of(slot, core)
        return remote(view, view, core_sem.at[0, slot], core_sem.at[1, slot], tp=mate)

    def take(slot):
        view = half_of(slot, 1 - core)
        remote(view, view, core_sem.at[0, slot], core_sem.at[1, slot], tp=mate).wait_recv()

    loads[0].wait()
    loads[1].wait()
    gather.open()
    pass_on = lambda slot: hand(slot).start()
    gather.other(0, pass_on)
    for dist in range(1, nf // 2):
        gather.step(dist, pass_on)
        gather.other(dist, pass_on)
    for load in loads[2:5]:
        load.wait()
    for k in range(1, nf):
        take((me + k) % nf)

    rows = jnp.dot(xv[...], fbuf[...], preferred_element_type=F32)
    terms = parts(rows, 2)
    for p in range(2):
        total = 0.0
        for term in terms:
            total = total + lax.dot_general(
                term[:, p * rank : (p + 1) * rank], cv[p], (((0,), (0,)), ((), ())), preferred_element_type=F32
            )
        rl[p * rank : (p + 1) * rank, :] = total

    def piece(slot):
        return pl.ds(pl.multiple_of(slot * pr, pr), pr)

    def scatter(k):
        to = (me + k) % nf
        return remote(rl.at[piece(to), :], rs.at[me], rs_sem.at[0, k], rs_sem.at[1, me], fs=to)

    for k in range(1, nf):
        scatter(k).start()
    summed = rl[piece(me), :]
    for k in range(1, nf):
        frm = (me + k) % nf
        remote(rl.at[piece(me), :], rs.at[frm], rs_sem.at[0, k], rs_sem.at[1, frm], fs=frm).wait_recv()
        summed = summed + rs[frm]
    rfull[piece(me), :] = summed

    def spread(k):
        view = rfull.at[piece(me), :]
        return remote(view, view, ag_sem.at[0, k], ag_sem.at[1, me], fs=(me + k) % nf)

    for k in range(1, nf):
        spread(k).start()
    for load in loads[5:]:
        load.wait()
    for k in range(1, nf):
        frm = (me + k) % nf
        view = rfull.at[piece(frm), :]
        remote(view, view, ag_sem.at[0, k], ag_sem.at[1, frm], fs=frm).wait_recv()

    squares = jnp.zeros((), F32)
    directions = []
    for p in range(2):
        projected = rfull[p * rank : (p + 1) * rank, :]
        first_new, second_new, direction = update_moments(projected, m1[p], m2[p])
        fnv[p] = first_new
        snv[p] = second_new
        squares = squares + jnp.sum(direction * direction)
        directions.append(direction)
    ss[tp] = jnp.full(ss.shape[1:], squares, F32)

    def tell(k):
        return remote(ss.at[tp], ss.at[tp], ss_sem.at[0, k], ss_sem.at[1, tp], tp=(tp + k) % nt)

    for k in range(1, nt):
        tell(k).start()
    raw = []
    for p in range(2):
        own = fbuf[block(me), p * rank : (p + 1) * rank]
        total = 0.0
        for term in reversed(parts(directions[p], 3)):
            total = total + jnp.dot(own, term, preferred_element_type=F32)
        raw.append(total)
    for k in range(1, nt):
        frm = (tp + k) % nt
        remote(ss.at[frm], ss.at[frm], ss_sem.at[0, k], ss_sem.at[1, frm], tp=frm).wait_recv()
    total = ss[0]
    for t in range(1, nt):
        total = total + ss[t]
    entries = 2 * rank * directions[0].shape[1] * nt
    scale = (learn_rate / jnp.sqrt(total / entries + 1e-06))[0:1, 0:1]

    cut = depth // SPLIT

    def rows_of(slot, part):
        return pl.ds(pl.multiple_of(slot * depth + part * cut, cut), cut)

    lines = []
    for p in range(2):
        step = -scale * raw[p]
        new = wv[p] + step
        cbuf[p] = new.astype(BF)
        stv[p] = step
        nwv[p] = new
        for part in range(SPLIT):
            i = p * SPLIT + part
            own = cbuf.at[p, part * cut : (part + 1) * cut, :]
            piece_of = functools.partial(lambda p, part, slot: copy_out[p].at[rows_of(slot, part), :], p, part)
            lines.append(Line(nf, me, own, piece_of, *(cp_sem.at[i, j] for j in range(4)), shift=p == 1))
            lines[i].open()
    outs = []
    for i, (src, dst) in enumerate(((fnv, first_out), (snv, second_out), (stv, step_out), (nwv, new_out))):
        outs += [pltpu.make_async_copy(src.at[p], dst[p], out_sem.at[2 * i + p]) for p in range(2)]
    for p in range(2):
        outs += [pltpu.make_async_copy(cbuf.at[p], copy_out[p].at[block(me), :], out_sem.at[8 + p])]
    for out in outs:
        out.start()
    at_end = (me // 2 == 0) | (me // 2 == nf // 2 - 1)

    def pairs():
        for line in lines:
            line.other(0)

    for dist in range(1, nf // 2):
        for line in lines:
            line.step(dist)
        if dist == 1:
            pl.when(at_end)(pairs)
    pl.when(jnp.logical_not(at_end))(pairs)
    for dist in range(1, nf // 2):
        for line in lines:
            line.other(dist)

    gather.close()
    for line in lines:
        line.close()
    for k in range(1, nf):
        hand((me + k) % nf).wait_send()
        scatter(k).wait_send()
        spread(k).wait_send()
    for k in range(1, nt):
        tell(k).wait_send()
    for out in outs:
        out.wait()


def out_kernel(n, *refs):
    copies = [pltpu.make_async_copy(refs[i], refs[n + i], refs[2 * n].at[i]) for i in range(n)]
    for copy in copies:
        copy.start()
    for copy in copies:
        copy.wait()


def fused(nf, nt, *args):
    x, cot, factor, weight, first = args[0], args[1], args[3], args[5], args[7]
    tokens, width = cot.shape
    depth, rank = factor.shape
    pr = 2 * rank // nf
    shape = jax.ShapeDtypeStruct
    outs = [shape(weight.shape, F32)] * 4 + [shape((nf * depth, width), BF)] * 2 + [shape(first.shape, F32)] * 4
    anywhere, hbm = pl.BlockSpec(memory_space=pl.ANY), pl.BlockSpec(memory_space=pltpu.HBM)
    vmem, dma = pltpu.VMEM, pltpu.SemaphoreType.DMA
    results = pl.pallas_call(
        functools.partial(main_kernel, nf, nt),
        out_shape=outs,
        in_specs=[hbm] * 11,
        out_specs=[anywhere] * 10,
        scratch_shapes=[
            vmem(x.shape, BF),
            vmem((2, tokens, width), BF),
            vmem((nf * depth, 2 * rank), BF),
            vmem((2 * rank, width), F32),
            vmem((nf, pr, width), F32),
            vmem((2 * rank, width), F32),
            vmem((nt, 8, 128), F32),
            vmem((2, depth, width), F32),
            vmem((2, rank, width), F32),
            vmem((2, rank, width), F32),
            vmem((2, depth, width), F32),
            vmem((2, depth, width), F32),
            vmem((2, rank, width), F32),
            vmem((2, rank, width), F32),
            vmem((2, depth, width), BF),
            dma((11,)),
            dma((10,)),
            dma((4, nf)),
            dma((2, nf)),
            dma((2, nf)),
            dma((2, nf)),
            dma((2, nt)),
            dma((2 * SPLIT, 4, nf)),
        ],
        compiler_params=pltpu.CompilerParams(
            collective_id=0, has_side_effects=True, vmem_limit_bytes=24 * 1024 * 1024
        ),
    )(*[pltpu.with_memory_space_constraint(a, pltpu.HBM) for a in args])
    return pl.pallas_call(
        functools.partial(out_kernel, len(outs)),
        out_shape=outs,
        in_specs=[anywhere] * 10,
        out_specs=[hbm] * 10,
        scratch_shapes=[dma((len(outs),))],
        compiler_params=pltpu.CompilerParams(vmem_limit_bytes=1024 * 1024),
    )(*results)


def fits(nf, nt, depth, rank):
    return nf % 2 == 0 and nt % 2 == 0 and nf <= 16 and depth % (16 * SPLIT) == 0 and (2 * rank) % (8 * nf) == 0


def device_step(nf, nt, *args):
    depth, rank = args[3].shape
    if fits(nf, nt, depth, rank):
        return tuple(fused(nf, nt, *args))
    return local(*args)


def solution(mesh):
    return jax.shard_map(
        functools.partial(device_step, mesh.shape["fs"], mesh.shape["tp"]),
        mesh=mesh,
        in_specs=(
            P("fs", None),
            P("fs", "tp"),
            P("fs", "tp"),
            P("fs", None),
            P("fs", None),
            P("fs", "tp"),
            P("fs", "tp"),
            P(None, "tp"),
            P(None, "tp"),
            P(None, "tp"),
            P(None, "tp"),
        ),
        out_specs=(
            P("fs", "tp"),
            P("fs", "tp"),
            P("fs", "tp"),
            P("fs", "tp"),
            P(None, "tp"),
            P(None, "tp"),
            P(None, "tp"),
            P(None, "tp"),
            P(None, "tp"),
            P(None, "tp"),
        ),
        check_vma=False,
    )
```
